1024 devices in a mesh: rep: 8 (over y), fs: 32 (over z, x_hi), tp: 4 (over x_lo, core).
Axes of the slice: x: 8 (x_hi: 4, x_lo: 2; x = x_hi * 2 + x_lo), y: 8, z: 8, core: 2. Of those that a mesh axis runs over, the one named last changes fastest.
Arguments:
- tokens: bfloat16 [256, 192, 2048], P(('rep', 'fs'), None, 'tp'), may hold values from -40 to 40
- ff_first: bfloat16 [2048, 2048], P('fs', 'tp'), may hold values from -0.125 to 0.125
- ff_second: bfloat16 [2048, 2048], P('fs', 'tp'), may hold values from -0.125 to 0.125
- ff_down: bfloat16 [2048, 2048], P('fs', 'tp'), may hold values from -0.125 to 0.125
- mix_stream: bfloat16 [2048, 2048], P('fs', 'tp'), may hold values from -0.125 to 0.125
- mix_gate: bfloat16 [2048, 2048], P('fs', 'tp'), may hold values from -0.125 to 0.125
- mix_down: bfloat16 [2048, 2048], P('fs', 'tp'), may hold values from -0.125 to 0.125
- gain_one: float32 [2048], P('tp'), may hold values from 0.1 to 1.9
- gain_two: float32 [2048], P('tp'), may hold values from 0.1 to 1.9
- gain_three: float32 [2048], P('tp'), may hold values from 0.1 to 1.9
Outputs:
- layer_out: bfloat16 [256, 192, 2048], P(('rep', 'fs'), None, 'tp')
The draws below stay inside these ranges and needn't reach their ends.
All inputs are finite; a program needn't handle non-finite values.
Results may differ from the reference program's by a relative error of at most 0.01.
Values may be sent and summed in bfloat16 or wider, within the bound.
No kernel may reach another device: no remote copies, remote signals or barrier semaphores. Data moves between devices by JAX's collectives and lax.ppermute only.
A program may use at most 64 MiB of HBM per device.

```python
import jax
import jax.numpy as jnp
from jax import lax

D = 2048
FF = 2048
SEQ = 192
BATCH = 256


def draw_tokens(key, part):
    normal_draw = jax.random.truncated_normal(key, -5.0, 5.0, (BATCH, SEQ, D), jnp.float32)
    column_ramp = jnp.arange(D, dtype=jnp.float32) / D
    values = normal_draw * 0.6 * 3.0 ** column_ramp[None, None, :]
    return values.astype(jnp.bfloat16)


def level_of(own_key, shape, cuts, smallest, largest):
    def one(axis_at, blocks):
        draws = jax.random.uniform(jax.random.fold_in(jax.random.fold_in(own_key, 6), axis_at), (blocks,), jnp.float32, smallest / len(cuts), largest / len(cuts))
        return jnp.repeat(jnp.exp(draws), shape[axis_at] // blocks).reshape((-1,) + (1,) * (len(shape) - axis_at - 1))

    level = one(*cuts[0])
    for cut in cuts[1:]:
        level = level * one(*cut)
    return level


def bell_draw(key, extent, deviation, bound, cuts=(), kind=jnp.bfloat16):
    array = jax.random.normal(key, extent, jnp.float32) * deviation
    if len(cuts) > 0:
        array = level_of(key, extent, cuts, -0.22, 0.18) * array
    return jnp.clip(array, min=-bound, max=bound).astype(kind)


def setup_inputs(seed: int = 0) -> dict:
    splits = jax.random.split(jax.random.key(seed), 11)
    tokens = draw_tokens(jax.random.fold_in(splits[10], 71), 0)
    ff_first = bell_draw(splits[1], (D, FF), D ** -0.5, 0.125, ((0, 32), (1, 4)))
    ff_second = bell_draw(splits[2], (D, FF), D ** -0.5, 0.125, ((0, 32), (1, 4)))
    ff_down = bell_draw(splits[3], (FF, D), FF ** -0.5, 0.125, ((0, 32), (1, 4)))
    mix_stream = bell_draw(splits[4], (D, D), D ** -0.5, 0.125, ((0, 32), (1, 4)))
    mix_gate = bell_draw(splits[5], (D, D), D ** -0.5, 0.125, ((0, 32), (1, 4)))
    mix_down = bell_draw(splits[6], (D, D), D ** -0.5, 0.125, ((0, 32), (1, 4)))
    gain_one = jnp.clip(1.0 + 0.18 * jax.random.normal(splits[7], (D,), jnp.float32), 0.1, 1.9)
    gain_two = jnp.clip(1.0 + 0.18 * jax.random.normal(splits[8], (D,), jnp.float32), 0.1, 1.9)
    gain_three = jnp.clip(1.0 + 0.18 * jax.random.normal(splits[9], (D,), jnp.float32), 0.1, 1.9)
    return dict(tokens=tokens, ff_first=ff_first, ff_second=ff_second, ff_down=ff_down, mix_stream=mix_stream, mix_gate=mix_gate, mix_down=mix_down, gain_one=gain_one, gain_two=gain_two, gain_three=gain_three)


alpha_scale = 2.0 ** 0.5
norm_eps = 1e-05

def matmul(inputs, weight):
    flat_rows = inputs.reshape(-1, inputs.shape[-1])
    result = jnp.dot(flat_rows, weight, preferred_element_type=jnp.float32)
    return result.reshape(inputs.shape[:-1] + (weight.shape[1],))

def layer_norm(summed, gain_vec):
    row_mean = lax.optimization_barrier(jnp.mean(summed, axis=-1, keepdims=True))
    row_var = lax.optimization_barrier(jnp.mean(jnp.square(summed - row_mean), axis=-1, keepdims=True))
    normed = (summed - row_mean) * lax.rsqrt(row_var + norm_eps)
    return (normed * gain_vec.astype(jnp.float32)).astype(jnp.bfloat16)

def half_step(inputs, first_w, second_w, down_w, gain_vec):
    hidden = (jax.nn.silu(matmul(inputs, first_w)) * matmul(inputs, second_w)).astype(jnp.bfloat16)
    return layer_norm(alpha_scale * inputs.astype(jnp.float32) + 0.5 * matmul(hidden, down_w), gain_vec)

def pool_mix(inputs, stream_w, gate_w, down_w, gain_vec):
    stream = matmul(inputs, stream_w).astype(jnp.bfloat16)
    gate_act = matmul(inputs, gate_w)
    length = stream.shape[1]
    width = stream.shape[2]
    running = jnp.cumsum(stream.astype(jnp.float32), axis=1)
    positions = jnp.arange(length)
    channel_group = jnp.arange(width) * 4 // width
    pooled = jnp.zeros_like(running)
    for scale_level in range(4):
        window = 2 << scale_level
        lagged = jnp.pad(running, ((0, 0), (window, 0), (0, 0)))[:, :length]
        counts = jnp.minimum(positions + 1, window).astype(jnp.float32)
        window_mean = (running - lagged) / counts[None, :, None]
        pooled = jnp.where((channel_group == scale_level)[None, None, :], window_mean, pooled)
    pooled = pooled - stream.astype(jnp.float32)
    mixed_rows = (pooled * jax.nn.silu(gate_act)).astype(jnp.bfloat16)
    return layer_norm(alpha_scale * inputs.astype(jnp.float32) + matmul(mixed_rows, down_w), gain_vec)

def reference(tokens, ff_first, ff_second, ff_down, mix_stream, mix_gate, mix_down, gain_one, gain_two, gain_three):
    first = half_step(tokens, ff_first, ff_second, ff_down, gain_one)
    second = pool_mix(first, mix_stream, mix_gate, mix_down, gain_two)
    return half_step(second, ff_first, ff_second, ff_down, gain_three)
```

```python
import functools

import jax
import jax.numpy as jnp
from jax import lax
from jax.experimental import pallas as pl
from jax.experimental.pallas import tpu as pltpu
from jax.sharding import Mesh
from jax.sharding import PartitionSpec as P

alpha_scale = 2.0**0.5
norm_eps = 1e-05
BF = jnp.bfloat16
F32 = jnp.float32

SEQ = 192
D = 2048
LOC = 512
PAY = 640
NZ = 8
NX = 4
KB = 256
SUB = 64


def _rows(ref, base, cols):
    xh = lax.axis_index("xh")
    parts = []
    for q in range(NX):
        at = base + lax.rem(q - xh + NX, NX) * SUB
        parts.append(ref[pl.ds(pl.multiple_of(at, SUB), SUB), cols])
    return jnp.concatenate(parts, axis=0)


def _dot(a, b):
    return jnp.dot(a, b, preferred_element_type=F32)


def _product_whole(h_ref, w_ref, col):
    acc = None
    for zb in range(NZ):
        part = _dot(h_ref[:, zb * KB : (zb + 1) * KB], _rows(w_ref, zb * KB, slice(col, col + LOC)))
        acc = part if acc is None else acc + part
    return acc


def _product_ring(h_ref, blocks, col):
    y = lax.axis_index("rep")
    z = lax.axis_index("z")
    acc = None
    for k in range(NZ):
        zb = lax.rem(z + y + k, NZ)
        h = h_ref[:, pl.ds(pl.multiple_of(zb * KB, KB), KB)]
        part = _dot(h, _rows(blocks[k], 0, slice(col, col + LOC)))
        acc = part if acc is None else acc + part
    return acc


def _tp_index():
    return lax.axis_index("xl") * 2 + lax.axis_index("co")


def _normed(pay_ref, gain_ref, h_ref):
    cents, parts, sums = [], [], None
    for j in range(4):
        zc = pay_ref[:, j * PAY : j * PAY + LOC].astype(F32)
        tail = pay_ref[:, j * PAY + LOC : (j + 1) * PAY].astype(F32)
        cent = jnp.sum(tail, axis=1, keepdims=True)
        s = jnp.sum(zc, axis=1, keepdims=True) + LOC * cent
        sums = s if sums is None else sums + s
        cents.append(cent)
    mean = sums / D
    var = None
    for j in range(4):
        zc = pay_ref[:, j * PAY : j * PAY + LOC].astype(F32)
        dev = zc + (cents[j] - mean)
        v = jnp.sum(dev * dev, axis=1, keepdims=True)
        var = v if var is None else var + v
    scale = lax.rsqrt(var / D + norm_eps)
    for j in range(4):
        zc = pay_ref[:, j * PAY : j * PAY + LOC].astype(F32)
        dev = zc + (cents[j] - mean)
        g = gain_ref[:, j * LOC : (j + 1) * LOC]
        h_ref[:, j * LOC : (j + 1) * LOC] = (dev * scale * g).astype(BF)


def _payload(total, out_ref):
    cent = jnp.sum(total, axis=1, keepdims=True) / LOC
    out_ref[:, :LOC] = (total - cent).astype(BF)
    hi = cent.astype(BF).astype(F32)
    rest = cent - hi
    mid = rest.astype(BF).astype(F32)
    low = rest - mid
    lane = lax.broadcasted_iota(jnp.int32, (SEQ, PAY - LOC), 1)
    tail = jnp.where(lane == 0, hi, jnp.where(lane == 1, mid, jnp.where(lane == 2, low, 0.0)))
    out_ref[:, LOC:] = tail.astype(BF)


def _own(h_ref):
    return h_ref[:, pl.ds(pl.multiple_of(_tp_index() * LOC, LOC), LOC)]


def _ff_in_first(h_ref, w1_ref, *rest):
    blocks, out_ref = rest[:NZ], rest[NZ]
    a = _product_whole(h_ref, w1_ref, 0)
    b = _product_ring(h_ref, blocks, 0)
    out_ref[...] = (jax.nn.silu(a) * b).astype(BF)


def _ff_in_normed(pay_ref, gain_ref, w1_ref, *rest):
    blocks, out_ref, own_ref, h_ref = rest[:NZ], rest[NZ], rest[NZ + 1], rest[NZ + 2]
    _normed(pay_ref, gain_ref, h_ref)
    own_ref[...] = _own(h_ref)
    a = _product_whole(h_ref, w1_ref, 0)
    b = _product_ring(h_ref, blocks, 0)
    out_ref[...] = (jax.nn.silu(a) * b).astype(BF)


def _down(factor, hid_ref, own_ref, *rest):
    blocks, out_ref = rest[:NZ], rest[NZ]
    acc = _product_ring(hid_ref, blocks, 0)
    _payload(alpha_scale * own_ref[...].astype(F32) + factor * acc, out_ref)


def _down_last(hid_ref, own_ref, *rest):
    blocks, out_ref, stat_ref = rest[:NZ], rest[NZ], rest[NZ + 1]
    acc = _product_ring(hid_ref, blocks, 0)
    total = alpha_scale * own_ref[...].astype(F32) + 0.5 * acc
    out_ref[...] = total
    cent = jnp.sum(total, axis=1, keepdims=True) / LOC
    dev = total - cent
    square = jnp.sum(dev * dev, axis=1, keepdims=True)
    lane = lax.broadcasted_iota(jnp.int32, (SEQ, 128), 1)
    stat_ref[...] = jnp.where(lane == 0, cent, jnp.where(lane == 1, square, 0.0))


def _mix_in(pay_ref, gain_ref, w_ref, out_ref, own_ref, h_ref):
    _normed(pay_ref, gain_ref, h_ref)
    own_ref[...] = _own(h_ref)
    stream = _product_whole(h_ref, w_ref, 0).astype(BF)
    gate = _product_whole(h_ref, w_ref, LOC)
    window = lax.shift_left(jnp.int32(2), _tp_index())
    later = lax.broadcasted_iota(jnp.int32, (SEQ, SEQ), 0)
    earlier = lax.broadcasted_iota(jnp.int32, (SEQ, SEQ), 1)
    offset = later - earlier
    band = jnp.where((offset >= 0) & (offset < window), 1.0, 0.0).astype(BF)
    sums = _dot(band, stream)
    row = lax.broadcasted_iota(jnp.int32, (SEQ, 1), 0)
    counts = jnp.minimum(row + 1, window).astype(F32)
    pooled = sums / counts - stream.astype(F32)
    out_ref[...] = (pooled * jax.nn.silu(gate)).astype(BF)


def _call(kernel, outs, scratch, flops, *args):
    full = pl.BlockSpec(memory_space=pltpu.VMEM)
    return pl.pallas_call(
        kernel,
        out_shape=outs,
        in_specs=[full] * len(args),
        out_specs=jax.tree.map(lambda _: full, outs),
        scratch_shapes=scratch,
        cost_estimate=pl.CostEstimate(flops=flops, bytes_accessed=0, transcendentals=0),
        compiler_params=pltpu.CompilerParams(vmem_limit_bytes=12 * 1024 * 1024),
    )(*args)


def _sds(cols, dtype=BF):
    return jax.ShapeDtypeStruct((SEQ, cols), dtype)


H_SCRATCH = [pltpu.VMEM((SEQ, D), BF)]
ONE = 2 * SEQ * D * LOC


def _shift(value, axis, by):
    n = lax.axis_size(axis)
    return lax.ppermute(value, axis, [(i, (i + by) % n) for i in range(n)])


def _diagonal(value):
    pairs = [(y * NZ + (z + y) % NZ, y * NZ + z) for y in range(8) for z in range(NZ)]
    return lax.ppermute(value, ("rep", "z"), pairs)


def _x_blocks(value, opposite_from_left):
    left = _shift(value, "xh", 1)
    right = _shift(value, "xh", -1)
    far = _shift(left, "xh", 1) if opposite_from_left else _shift(right, "xh", -1)
    return jnp.concatenate([value, right, far, left], axis=0)


def _x_pair(a, b):
    both = jnp.concatenate([a, b], axis=1)
    n = a.shape[1]
    left = _shift(both, "xh", 1)
    right = _shift(both, "xh", -1)
    far_a = _shift(left[:, :n], "xh", 1)
    far_b = _shift(right[:, n:], "xh", -1)
    cat = lambda *v: jnp.concatenate(v, axis=0)
    return (
        cat(a, right[:, :n], far_a, left[:, :n]),
        cat(b, right[:, n:], far_b, left[:, n:]),
    )


def _y_ring(block):
    blocks = [None] * 8
    blocks[0] = block
    up = down = block
    for s in range(1, 5):
        down = _shift(down, "rep", -1)
        blocks[s] = down
        if s < 4:
            up = _shift(up, "rep", 1)
            blocks[8 - s] = up
    return blocks


def _whole(local_rows):
    return lax.all_gather(local_rows, ("xl", "co"), axis=1, tiled=True)


def shards(
    tokens, ff_first, ff_second, ff_down, mix_stream, mix_gate, mix_down, gain_one, gain_two, gain_three
):
    tok = tokens[0]
    diag = _diagonal(jnp.concatenate([ff_second, ff_down, mix_down], axis=1))
    second_d, down_d, mixd_d = diag[:, :LOC], diag[:, LOC : 2 * LOC], diag[:, 2 * LOC :]

    first_x, second_x = _x_pair(ff_first, second_d)
    w_first = lax.all_gather(first_x, "z", axis=0, tiled=True)
    second_ring = _y_ring(second_x)

    mix_x, rest_x = _x_pair(
        jnp.concatenate([mix_stream, mix_gate], axis=1), jnp.concatenate([down_d, mixd_d], axis=1)
    )
    w_mix = lax.all_gather(mix_x, "z", axis=0, tiled=True)
    down_ring = _y_ring(rest_x[:, :LOC])
    mixd_ring = _y_ring(rest_x[:, LOC:])

    gains = lax.all_gather(jnp.stack([gain_one, gain_two]), ("xl", "co"), axis=1, tiled=True)

    whole = _whole(tok)
    hidden = _call(_ff_in_first, _sds(LOC), [], 2 * ONE, whole, w_first, *second_ring)
    pay = _call(functools.partial(_down, 0.5), _sds(PAY), [], ONE, _whole(hidden), tok, *down_ring)

    gated, first = _call(
        _mix_in, (_sds(LOC), _sds(LOC)), H_SCRATCH, 2 * ONE, _whole(pay), gains[:1], w_mix
    )
    pay = _call(functools.partial(_down, 1.0), _sds(PAY), [], ONE, _whole(gated), first, *mixd_ring)

    hidden, second = _call(
        _ff_in_normed, (_sds(LOC), _sds(LOC)), H_SCRATCH, 2 * ONE,
        _whole(pay), gains[1:], w_first, *second_ring,
    )
    total, stats = _call(
        _down_last, (_sds(LOC, F32), _sds(128, F32)), [], ONE, _whole(hidden), second, *down_ring
    )

    every = lax.all_gather(stats[:, :2].T, ("xl", "co"), axis=0, tiled=False)
    cents, squares = every[:, 0], every[:, 1]
    mean = jnp.mean(cents, axis=0)
    var = (jnp.sum(squares, axis=0) + LOC * jnp.sum((cents - mean) ** 2, axis=0)) / D
    out = (total - mean[:, None]) * lax.rsqrt(var + norm_eps)[:, None] * gain_three[None, :]
    return out.astype(BF)[None]


def solution(mesh):
    fine = Mesh(mesh.devices.reshape(8, NZ, NX, 2, 2), ("rep", "z", "xh", "xl", "co"))
    rows, cols = ("z", "xh"), ("xl", "co")
    placed = (P(("rep", "z", "xh"), None, cols),) + (P(rows, cols),) * 6 + (P(cols),) * 3
    return jax.shard_map(
        shards, mesh=fine, in_specs=placed, out_specs=P(("rep", "z", "xh"), None, cols), check_vma=False
    )
```

```python
import functools

import jax
import jax.numpy as jnp
from jax import lax
from jax.experimental import pallas as pl
from jax.experimental.pallas import tpu as pltpu
from jax.sharding import Mesh
from jax.sharding import PartitionSpec as P


alpha_scale = 2.0**0.5
norm_eps = 1e-05
BF = jnp.bfloat16
F32 = jnp.float32

SEQ = 192
D = 2048
LOC = 512
PAY = 640
NZ = 8
NX = 4
KB = 256
GZ = 256


def _dot(a, b):
    return jnp.dot(a, b, preferred_element_type=F32)


def _product_whole(h_ref, w_ref, col, width, wait=None):
    acc = None
    for k in range(NZ):
        if wait is not None:
            wait[k].wait()
        rows = slice(k * KB, (k + 1) * KB)
        part = _dot(h_ref[:, rows], w_ref[rows, col : col + width])
        acc = part if acc is None else acc + part
    return acc


def _product_ring(h_ref, blocks, col, width, wait=None):
    y = lax.axis_index("rep")
    z = lax.axis_index("z")
    acc = None
    for k in range(NZ):
        if wait is not None:
            wait[k].wait()
        zb = lax.rem(z + y + k, NZ)
        h = h_ref[:, pl.ds(pl.multiple_of(zb * KB, KB), KB)]
        part = _dot(h, blocks[k][:, col : col + width])
        acc = part if acc is None else acc + part
    return acc


def _tp_index():
    return lax.axis_index("xl") * 2 + lax.axis_index("co")


def _gain(gain_ref, row, j):
    at = slice(j * LOC, (j + 1) * LOC)
    term = lambda i: gain_ref[row + i : row + i + 1, at].astype(F32)
    return term(0) + term(1) + term(2)


def _normed(pay_ref, gain_ref, row, h_ref):
    cents, sums = [], None
    for j in range(4):
        zc = pay_ref[:, j * PAY : j * PAY + LOC].astype(F32)
        tail = pay_ref[:, j * PAY + LOC : (j + 1) * PAY].astype(F32)
        cent = jnp.sum(tail, axis=1, keepdims=True)
        s = jnp.sum(zc, axis=1, keepdims=True) + LOC * cent
        sums = s if sums is None else sums + s
        cents.append(cent)
    mean = sums / D
    var = None
    for j in range(4):
        zc = pay_ref[:, j * PAY : j * PAY + LOC].astype(F32)
        dev = zc + (cents[j] - mean)
        v = jnp.sum(dev * dev, axis=1, keepdims=True)
        var = v if var is None else var + v
    scale = lax.rsqrt(var / D + norm_eps)
    for j in range(4):
        zc = pay_ref[:, j * PAY : j * PAY + LOC].astype(F32)
        dev = zc + (cents[j] - mean)
        g = _gain(gain_ref, row, j)
        h_ref[:, j * LOC : (j + 1) * LOC] = (dev * scale * g).astype(BF)


def _payload(total, out_ref):
    cent = jnp.sum(total, axis=1, keepdims=True) / LOC
    out_ref[:, :LOC] = (total - cent).astype(BF)
    hi = cent.astype(BF).astype(F32)
    rest = cent - hi
    mid = rest.astype(BF).astype(F32)
    low = rest - mid
    lane = lax.broadcasted_iota(jnp.int32, (SEQ, PAY - LOC), 1)
    tail = jnp.where(lane == 0, hi, jnp.where(lane == 1, mid, jnp.where(lane == 2, low, 0.0)))
    out_ref[:, LOC:] = tail.astype(BF)


def _own(h_ref):
    return h_ref[:, pl.ds(pl.multiple_of(_tp_index() * LOC, LOC), LOC)]


def _ff_in_first(tok_ref, w_ref, out_ref):
    h_ref = tok_ref.at[:SEQ]
    a = _product_whole(h_ref, w_ref, 0, LOC)
    b = _product_whole(h_ref, w_ref, LOC, LOC)
    out_ref[...] = (jax.nn.silu(a) * b).astype(BF)


def _ff_in_normed(pay_ref, gain_ref, w_ref, out_ref, own_ref, h_ref):
    _normed(pay_ref, gain_ref, 3, h_ref)
    own_ref[...] = _own(h_ref)
    a = _product_whole(h_ref, w_ref, 0, LOC)
    b = _product_whole(h_ref, w_ref, LOC, LOC)
    out_ref[...] = (jax.nn.silu(a) * b).astype(BF)


def _down(factor, col, hid_ref, own_ref, *rest):
    blocks, (out_ref,) = rest[:NZ], rest[NZ:]
    acc = _product_ring(hid_ref, blocks, col, LOC)
    _payload(alpha_scale * own_ref[...].astype(F32) + factor * acc, out_ref)


def _down_last(col, hid_ref, own_ref, *rest):
    blocks, (out_ref, stat_ref) = rest[:NZ], rest[NZ:]
    acc = _product_ring(hid_ref, blocks, col, LOC)
    total = alpha_scale * own_ref[...].astype(F32) + 0.5 * acc
    out_ref[...] = total
    cent = jnp.sum(total, axis=1, keepdims=True) / LOC
    dev = total - cent
    square = jnp.sum(dev * dev, axis=1, keepdims=True)
    lane = lax.broadcasted_iota(jnp.int32, (SEQ, 128), 1)
    stat_ref[...] = jnp.where(lane == 0, cent, jnp.where(lane == 1, square, 0.0))


def _mix_in(pay_ref, gain_ref, w_ref, *rest):
    blocks, (out_ref, own_ref, h_ref, along_z, along_y, sems) = rest[:NZ], rest[NZ:]
    z_copies, y_copies = [], []
    for k in range(NZ):
        rows = slice(k * KB, (k + 1) * KB)
        z_copies.append(pltpu.make_async_copy(w_ref.at[rows], along_z.at[rows], sems.at[0, k]))
        gate = blocks[k].at[:, 2 * LOC :]
        y_copies.append(pltpu.make_async_copy(gate, along_y.at[k], sems.at[1, k]))
    for copy in z_copies + y_copies:
        copy.start()
    _normed(pay_ref, gain_ref, 0, h_ref)
    own_ref[...] = _own(h_ref)
    both = _product_whole(h_ref, along_z, 0, LOC + GZ, z_copies)
    stream = both[:, :LOC].astype(BF)
    rest_of_gate = _product_ring(
        h_ref, [along_y.at[k] for k in range(NZ)], 0, LOC - GZ, y_copies
    )
    gate = jnp.concatenate([both[:, LOC:], rest_of_gate], axis=1)
    window = lax.shift_left(jnp.int32(2), _tp_index())
    later = lax.broadcasted_iota(jnp.int32, (SEQ, SEQ), 0)
    earlier = lax.broadcasted_iota(jnp.int32, (SEQ, SEQ), 1)
    offset = later - earlier
    band = jnp.where((offset >= 0) & (offset < window), 1.0, 0.0).astype(BF)
    sums = _dot(band, stream)
    row = lax.broadcasted_iota(jnp.int32, (SEQ, 1), 0)
    counts = jnp.minimum(row + 1, window).astype(F32)
    pooled = sums / counts - stream.astype(F32)
    out_ref[...] = (pooled * jax.nn.silu(gate)).astype(BF)


def _call(kernel, outs, scratch, flops, acts, weights, limit_mib=6, space=pltpu.VMEM):
    full = pl.BlockSpec(memory_space=pltpu.VMEM)
    return pl.pallas_call(
        kernel,
        out_shape=outs,
        in_specs=[full] * len(acts) + [pl.BlockSpec(memory_space=space)] * len(weights),
        out_specs=jax.tree.map(lambda _: full, outs),
        scratch_shapes=scratch,
        cost_estimate=pl.CostEstimate(flops=flops, bytes_accessed=0, transcendentals=0),
        compiler_params=pltpu.CompilerParams(vmem_limit_bytes=limit_mib * 1024 * 1024),
    )(*acts, *weights)


def _sds(cols, dtype=BF):
    return jax.ShapeDtypeStruct((SEQ, cols), dtype)


ONE = 2 * SEQ * D * LOC


def _shift(value, axis, by):
    n = lax.axis_size(axis)
    return lax.ppermute(value, axis, [(i, (i + by) % n) for i in range(n)])


def _diagonal(value):
    pairs = [(y * NZ + (z + y) % NZ, y * NZ + z) for y in range(8) for z in range(NZ)]
    return lax.ppermute(value, ("rep", "z"), pairs)


def _cat(*values, axis=1):
    return jnp.concatenate(values, axis=axis)


def _over_xh(*values):
    return lax.all_gather(_cat(*values), "xh", axis=0, tiled=True)


def _y_ring(block):
    blocks = [None] * 8
    blocks[0] = block
    up = down = block
    for s in range(1, 5):
        down = _shift(down, "rep", -1)
        blocks[s] = down
        if s < 4:
            up = _shift(up, "rep", 1)
            blocks[8 - s] = up
    return blocks


def _whole(local_rows):
    return lax.all_gather(local_rows, ("xl", "co"), axis=1, tiled=True)


def _terms(gain):
    hi = lax.reduce_precision(gain, 8, 7)
    mid = lax.reduce_precision(gain - hi, 8, 7)
    return [t.astype(BF)[None] for t in (hi, mid, gain - hi - mid)]


def shards(
    tokens, ff_first, ff_second, ff_down, mix_stream, mix_gate, mix_down, gain_one, gain_two, gain_three
):
    tok = tokens[0]
    diag = _diagonal(_cat(ff_down, mix_down, mix_gate[:, GZ:]))
    x1 = _over_xh(ff_first, ff_second, mix_stream)
    w_ff = lax.all_gather(x1[:, : 2 * LOC], "z", axis=0, tiled=True)
    x2 = _over_xh(mix_gate[:, :GZ], diag)
    w_mix = lax.all_gather(_cat(x1[:, 2 * LOC :], x2[:, :GZ]), "z", axis=0, tiled=True)
    ring = _y_ring(x2[:, GZ:])

    gains = _terms(gain_one) + _terms(gain_two) + [jnp.zeros((10, LOC), BF)]
    whole = _whole(_cat(tok, *gains, axis=0))

    gains = whole[SEQ:]
    two = (_sds(LOC), _sds(LOC))
    h_scratch = [pltpu.VMEM((SEQ, D), BF)]

    hidden = _call(_ff_in_first, _sds(LOC), [], 2 * ONE, (whole,), (w_ff,))
    wide = _whole(hidden)
    down = functools.partial(_down, 0.5, 0)
    pay = _call(down, _sds(PAY), [], ONE, (wide, tok), ring)

    wide = _whole(pay)
    mix_scratch = h_scratch + [
        pltpu.VMEM((D, LOC + GZ), BF),
        pltpu.VMEM((NZ, KB, LOC - GZ), BF),
        pltpu.SemaphoreType.DMA((2, NZ)),
    ]
    gated, first = _call(
        _mix_in, two, mix_scratch, 2 * ONE, (wide, gains), (w_mix, *ring), 61, pltpu.HBM
    )
    wide = _whole(gated)
    down = functools.partial(_down, 1.0, LOC)
    pay = _call(down, _sds(PAY), [], ONE, (wide, first), ring)

    wide = _whole(pay)
    hidden, second = _call(_ff_in_normed, two, h_scratch, 2 * ONE, (wide, gains), (w_ff,))
    wide = _whole(hidden)
    last = functools.partial(_down_last, 0)
    sums = (_sds(LOC, F32), _sds(128, F32))
    total, stats = _call(last, sums, [], ONE, (wide, second), ring)

    every = lax.all_gather(stats[:, :2].T, ("xl", "co"), axis=0, tiled=False)
    cents, squares = every[:, 0], every[:, 1]
    mean = jnp.mean(cents, axis=0)
    var = (jnp.sum(squares, axis=0) + LOC * jnp.sum((cents - mean) ** 2, axis=0)) / D
    out = (total - mean[:, None]) * lax.rsqrt(var + norm_eps)[:, None] * gain_three[None, :]
    return out.astype(BF)[None]


def solution(mesh):
    fine = Mesh(mesh.devices.reshape(8, NZ, NX, 2, 2), ("rep", "z", "xh", "xl", "co"))
    rows, cols = ("z", "xh"), ("xl", "co")
    placed = (P(("rep", "z", "xh"), None, cols),) + (P(rows, cols),) * 6 + (P(cols),) * 3
    return jax.shard_map(
        shards, mesh=fine, in_specs=placed, out_specs=P(("rep", "z", "xh"), None, cols), check_vma=False
    )
```

```python
import jax
import jax.numpy as jnp
from jax import lax
from jax.experimental import pallas as pl
from jax.experimental.pallas import tpu as pltpu
from jax.sharding import Mesh
from jax.sharding import PartitionSpec as P


alpha_scale = 2.0**0.5
norm_eps = 1e-05
BF = jnp.bfloat16
F32 = jnp.float32

SEQ = 192
D = 2048
LOC = 512
ROWS = 208
NZ = 8
NX = 4
KB = 256


def _dot(a, b):
    return jnp.dot(a, b, preferred_element_type=F32)


def _product_whole(h_ref, w_ref, col, width, wait=None):
    acc = None
    for k in range(NZ):
        if wait is not None:
            wait[k].wait()
        rows = slice(k * KB, (k + 1) * KB)
        part = _dot(h_ref[:, rows], w_ref[rows, col : col + width])
        acc = part if acc is None else acc + part
    return acc


NEAR = (0, 1, 7, 2)
FAR = (3, 6, 4, 5)


def _product_ring(h_ref, near, far, col, width, wait=None):
    y = lax.axis_index("rep")
    z = lax.axis_index("z")
    acc = None
    for i, k in enumerate(NEAR + FAR):
        if wait is not None and i >= 4:
            wait[i - 4].wait()
        block = near[i] if i < 4 else far.at[i - 4]
        zb = lax.rem(z + y + k, NZ)
        h = h_ref[:, pl.ds(pl.multiple_of(zb * KB, KB), KB)]
        part = _dot(h, block[:, col : col + width])
        acc = part if acc is None else acc + part
    return acc


def _tp_index():
    return lax.axis_index("xl") * 2 + lax.axis_index("co")


def _gain(gain_ref, row, j):
    at = slice(j * LOC, (j + 1) * LOC)
    term = lambda i: gain_ref[row + i : row + i + 1, at].astype(F32)
    return term(0) + term(1) + term(2)


def _normed(pay_ref, gain_ref, row, h_ref):
    width = 2 * 128
    token = lax.broadcasted_iota(jnp.int32, (SEQ, width), 0)
    lane = lax.broadcasted_iota(jnp.int32, (SEQ, width), 1)
    cents, sums = [], None
    for j in range(4):
        zc = pay_ref[:SEQ, j * LOC : (j + 1) * LOC].astype(F32)
        terms = pay_ref[SEQ:, j * LOC : j * LOC + width].astype(F32)
        across = jnp.sum(terms, axis=0, keepdims=True)
        cent = jnp.sum(jnp.where(token == lane, across, 0.0), axis=1, keepdims=True)
        s = jnp.sum(zc, axis=1, keepdims=True) + LOC * cent
        sums = s if sums is None else sums + s
        cents.append(cent)
    mean = sums / D
    var = None
    for j in range(4):
        zc = pay_ref[:SEQ, j * LOC : (j + 1) * LOC].astype(F32)
        dev = zc + (cents[j] - mean)
        v = jnp.sum(dev * dev, axis=1, keepdims=True)
        var = v if var is None else var + v
    scale = lax.rsqrt(var / D + norm_eps)
    for j in range(4):
        zc = pay_ref[:SEQ, j * LOC : (j + 1) * LOC].astype(F32)
        dev = zc + (cents[j] - mean)
        g = _gain(gain_ref, row, j)
        h_ref[:, j * LOC : (j + 1) * LOC] = (dev * scale * g).astype(BF)


def _payload(total, out_ref):
    cent = jnp.sum(total, axis=1, keepdims=True) / LOC
    out_ref[:SEQ] = (total - cent).astype(BF)
    token = lax.broadcasted_iota(jnp.int32, (SEQ, LOC), 0)
    lane = lax.broadcasted_iota(jnp.int32, (SEQ, LOC), 1)
    across = jnp.sum(jnp.where(token == lane, cent, 0.0), axis=0, keepdims=True)
    hi, mid, low = _terms(across)
    line = lax.broadcasted_iota(jnp.int32, (ROWS - SEQ, LOC), 0)
    terms = jnp.where(line == 0, hi, jnp.where(line == 1, mid, jnp.where(line == 2, low, 0.0)))
    out_ref[SEQ:] = terms.astype(BF)


def _own(h_ref):
    return h_ref[:, pl.ds(pl.multiple_of(_tp_index() * LOC, LOC), LOC)]


def _ff_in_first(tok_ref, w_ref, out_ref, w, sems):
    copies = [[], []]
    for part, cols in enumerate((slice(0, 2 * LOC), slice(2 * LOC, 3 * LOC))):
        for k in range(NZ):
            at = (slice(k * KB, (k + 1) * KB), cols)
            copies[part].append(pltpu.make_async_copy(w_ref.at[at], w.at[at], sems.at[part, k]))
            copies[part][k].start()
    both = _product_whole(tok_ref.at[:SEQ], w, 0, 2 * LOC, copies[0])
    out_ref[...] = (jax.nn.silu(both[:, :LOC]) * both[:, LOC:]).astype(BF)
    for copy in copies[1]:
        copy.wait()


def _ff_in_normed(pay_ref, gain_ref, w_ref, out_ref, own_ref, h_ref):
    _normed(pay_ref, gain_ref, 3, h_ref)
    own_ref[...] = _own(h_ref)
    both = _product_whole(h_ref, w_ref, 0, 2 * LOC)
    out_ref[...] = (jax.nn.silu(both[:, :LOC]) * both[:, LOC:]).astype(BF)


def _ff_down(hid_ref, own_ref, w_ref, out_ref):
    acc = _product_whole(hid_ref, w_ref, 2 * LOC, LOC)
    _payload(alpha_scale * own_ref[...].astype(F32) + 0.5 * acc, out_ref)


def _mix_down(hid_ref, own_ref, *rest):
    near, (far_ref, out_ref) = rest[:4], rest[4:]
    acc = _product_ring(hid_ref, near, far_ref, 2 * LOC, LOC)
    _payload(alpha_scale * own_ref[...].astype(F32) + acc, out_ref)


def _down_last(hid_ref, own_ref, w_ref, out_ref, stat_ref):
    acc = _product_whole(hid_ref, w_ref, 2 * LOC, LOC)
    total = alpha_scale * own_ref[...].astype(F32) + 0.5 * acc
    out_ref[...] = total
    cent = jnp.sum(total, axis=1, keepdims=True) / LOC
    dev = total - cent
    square = jnp.sum(dev * dev, axis=1, keepdims=True)
    lane = lax.broadcasted_iota(jnp.int32, (SEQ, 128), 1)
    stat_ref[...] = jnp.where(lane == 0, cent, jnp.where(lane == 1, square, 0.0))


def _mix_in(pay_ref, gain_ref, *rest):
    near, blocks, (out_ref, own_ref, far_ref, h_ref, sems) = rest[:4], rest[4:NZ], rest[NZ:]
    copies = [pltpu.make_async_copy(blocks[i], far_ref.at[i], sems.at[i]) for i in range(4)]
    for copy in copies:
        copy.start()
    _normed(pay_ref, gain_ref, 0, h_ref)
    own_ref[...] = _own(h_ref)
    both = _product_ring(h_ref, near, far_ref, 0, 2 * LOC, copies)
    stream = both[:, :LOC].astype(BF)
    gate = both[:, LOC:]
    window = lax.shift_left(jnp.int32(2), _tp_index())
    later = lax.broadcasted_iota(jnp.int32, (SEQ, SEQ), 0)
    earlier = lax.broadcasted_iota(jnp.int32, (SEQ, SEQ), 1)
    offset = later - earlier
    band = jnp.where((offset >= 0) & (offset < window), 1.0, 0.0).astype(BF)
    sums = _dot(band, stream)
    row = lax.broadcasted_iota(jnp.int32, (SEQ, 1), 0)
    counts = jnp.minimum(row + 1, window).astype(F32)
    pooled = sums / counts - stream.astype(F32)
    out_ref[...] = (pooled * jax.nn.silu(gate)).astype(BF)


def _call(kernel, outs, scratch, flops, args, in_hbm=(), limit_mib=6):
    full = pl.BlockSpec(memory_space=pltpu.VMEM)
    far = pl.BlockSpec(memory_space=pltpu.HBM)
    args_bytes = sum(a.size * a.dtype.itemsize for a in (*args, *in_hbm))
    return pl.pallas_call(
        kernel,
        out_shape=outs,
        in_specs=[full] * len(args) + [far] * len(in_hbm),
        out_specs=jax.tree.map(lambda _: full, outs),
        scratch_shapes=scratch,
        cost_estimate=pl.CostEstimate(
            flops=flops, bytes_accessed=args_bytes, transcendentals=0
        ),
        compiler_params=pltpu.CompilerParams(vmem_limit_bytes=limit_mib * 1024 * 1024),
    )(*args, *in_hbm)


def _terms(row):
    hi = row.astype(BF).astype(F32)
    mid = (row - hi).astype(BF).astype(F32)
    return hi, mid, row - hi - mid


def _pack(tok_ref, one_ref, two_ref, out_ref):
    out_ref[:SEQ] = tok_ref[...]
    line = lax.broadcasted_iota(jnp.int32, (ROWS - SEQ, LOC), 0)
    below = jnp.zeros((ROWS - SEQ, LOC), F32)
    for i, term in enumerate(_terms(one_ref[...]) + _terms(two_ref[...])):
        below = jnp.where(line == i, term, below)
    out_ref[SEQ:] = below.astype(BF)


def _sds(cols, dtype=BF, rows=SEQ):
    return jax.ShapeDtypeStruct((rows, cols), dtype)


ONE = 2 * SEQ * D * LOC


def _shift(value, axis, by):
    n = lax.axis_size(axis)
    return lax.ppermute(value, axis, [(i, (i + by) % n) for i in range(n)])


def _diagonal(value):
    pairs = [(y * NZ + (z + y) % NZ, y * NZ + z) for y in range(8) for z in range(NZ)]
    return lax.ppermute(value, ("rep", "z"), pairs)


def _cat(*values, axis=1):
    return jnp.concatenate(values, axis=axis)


def _over_xh(value):
    return lax.all_gather(value, "xh", axis=0, tiled=True)


def _y_ring(block):
    blocks = [None] * 8
    blocks[0] = block
    up = down = block
    for s in range(1, 5):
        down = _shift(down, "rep", -1)
        blocks[s] = down
        if s < 4:
            up = _shift(up, "rep", 1)
            blocks[8 - s] = up
    return blocks


def _whole(local_rows):
    return lax.all_gather(local_rows, ("xl", "co"), axis=1, tiled=True)


def shards(
    tokens, ff_first, ff_second, ff_down, mix_stream, mix_gate, mix_down, gain_one, gain_two, gain_three
):
    tok = tokens[0]
    diag = _diagonal(_cat(mix_stream, mix_gate, mix_down))
    x1 = _over_xh(_cat(ff_first, ff_second, ff_down))
    w_ff = lax.all_gather(x1, "z", axis=0, tiled=True)
    ring = _y_ring(_over_xh(diag))

    block = _call(_pack, _sds(LOC, rows=ROWS), [], 0, (tok, gain_one[None], gain_two[None]))
    whole = _whole(block)

    gains = whole[SEQ:]
    two = (_sds(LOC), _sds(LOC))
    h_scratch = [pltpu.VMEM((SEQ, D), BF)]

    outs = (_sds(LOC), _sds(3 * LOC, rows=D))
    sems = [pltpu.SemaphoreType.DMA((2, NZ))]
    hidden, w_ff = _call(_ff_in_first, outs, sems, 2 * ONE, (whole,), (w_ff,), 44)
    wide = _whole(hidden)
    pay = _call(_ff_down, _sds(LOC, rows=ROWS), [], ONE, (wide, tok, w_ff))

    wide = _whole(pay)
    near, far = [ring[k] for k in NEAR], [ring[k] for k in FAR]
    outs = (*two, jax.ShapeDtypeStruct((4, KB, 3 * LOC), BF))
    scratch = h_scratch + [pltpu.SemaphoreType.DMA((4,))]
    gated, first, far = _call(_mix_in, outs, scratch, 2 * ONE, (wide, gains, *near), far, 6)
    wide = _whole(gated)
    pay = _call(_mix_down, _sds(LOC, rows=ROWS), [], ONE, (wide, first, *near, far))

    wide = _whole(pay)
    hidden, second = _call(_ff_in_normed, two, h_scratch, 2 * ONE, (wide, gains, w_ff))
    wide = _whole(hidden)
    sums = (_sds(LOC, F32), _sds(128, F32))
    total, stats = _call(_down_last, sums, [], ONE, (wide, second, w_ff))

    every = lax.all_gather(stats[:, :2].T, ("xl", "co"), axis=0, tiled=False)
    cents, squares = every[:, 0], every[:, 1]
    mean = jnp.mean(cents, axis=0)
    var = (jnp.sum(squares, axis=0) + LOC * jnp.sum((cents - mean) ** 2, axis=0)) / D
    out = (total - mean[:, None]) * lax.rsqrt(var + norm_eps)[:, None] * gain_three[None, :]
    return out.astype(BF)[None]


def solution(mesh):
    fine = Mesh(mesh.devices.reshape(8, NZ, NX, 2, 2), ("rep", "z", "xh", "xl", "co"))
    rows, cols = ("z", "xh"), ("xl", "co")
    placed = (P(("rep", "z", "xh"), None, cols),) + (P(rows, cols),) * 6 + (P(cols),) * 3
    return jax.shard_map(
        shards, mesh=fine, in_specs=placed, out_specs=P(("rep", "z", "xh"), None, cols), check_vma=False
    )
```

```python
import jax
import jax.numpy as jnp
from jax import lax
from jax.experimental import pallas as pl
from jax.experimental.pallas import tpu as pltpu
from jax.sharding import Mesh
from jax.sharding import PartitionSpec as P


alpha_scale = 2.0**0.5
norm_eps = 1e-05
BF = jnp.bfloat16
F32 = jnp.float32

SEQ = 192
D = 2048
LOC = 512
ROWS = 200
NZ = 8
NX = 4
KB = 256


def _dot(a, b):
    return jnp.dot(a, b, preferred_element_type=F32)


def _product_whole(h_ref, w_ref, col, width, wait=None):
    acc = None
    for k in range(NZ):
        if wait is not None:
            wait[k].wait()
        rows = slice(k * KB, (k + 1) * KB)
        part = _dot(h_ref[:, rows], w_ref[rows, col : col + width])
        acc = part if acc is None else acc + part
    return acc


NEAR = (0, 1, 7, 2)
FAR = (3, 6, 4, 5)


def _product_ring(h_ref, near, far, col, width, wait=None):
    y = lax.axis_index("rep")
    z = lax.axis_index("z")
    acc = None
    for i, k in enumerate(NEAR + FAR):
        if wait is not None and i >= 4:
            wait[i - 4].wait()
        block = near[i] if i < 4 else far.at[i - 4]
        zb = lax.rem(z + y + k, NZ)
        h = h_ref[:, pl.ds(pl.multiple_of(zb * KB, KB), KB)]
        part = _dot(h, block[:, col : col + width])
        acc = part if acc is None else acc + part
    return acc


def _tp_index():
    return lax.axis_index("xl") * 2 + lax.axis_index("co")


def _gain(gain_ref, row, j):
    at = slice(j * LOC, (j + 1) * LOC)
    term = lambda i: gain_ref[row + i : row + i + 1, at].astype(F32)
    return term(0) + term(1) + term(2)


def _normed(pay_ref, gain_ref, row, h_ref):
    width = 2 * 128
    token = lax.broadcasted_iota(jnp.int32, (SEQ, width), 0)
    lane = lax.broadcasted_iota(jnp.int32, (SEQ, width), 1)
    cents, locals_, inner = [], [], None
    for j in range(4):
        zc = pay_ref[:SEQ, j * LOC : (j + 1) * LOC].astype(F32)
        terms = pay_ref[SEQ:, j * LOC : j * LOC + width].astype(F32)
        across = jnp.sum(terms, axis=0, keepdims=True)
        cent = jnp.sum(jnp.where(token == lane, across, 0.0), axis=1, keepdims=True)
        rest = jnp.sum(zc, axis=1, keepdims=True) / LOC
        square = jnp.sum(zc * zc, axis=1, keepdims=True) - LOC * rest * rest
        inner = square if inner is None else inner + square
        cents.append(cent)
        locals_.append(cent + rest)
    mean = (locals_[0] + locals_[1] + locals_[2] + locals_[3]) / 4
    var = inner
    for local in locals_:
        var = var + LOC * (local - mean) * (local - mean)
    scale = lax.rsqrt(var / D + norm_eps)
    for j in range(4):
        zc = pay_ref[:SEQ, j * LOC : (j + 1) * LOC].astype(F32)
        dev = zc + (cents[j] - mean)
        g = _gain(gain_ref, row, j)
        h_ref[:, j * LOC : (j + 1) * LOC] = (dev * scale * g).astype(BF)


def _payload(total, out_ref):
    cent = jnp.sum(total, axis=1, keepdims=True) / LOC
    out_ref[:SEQ] = (total - cent).astype(BF)
    token = lax.broadcasted_iota(jnp.int32, (SEQ, LOC), 0)
    lane = lax.broadcasted_iota(jnp.int32, (SEQ, LOC), 1)
    across = jnp.sum(jnp.where(token == lane, cent, 0.0), axis=0, keepdims=True)
    hi, mid, low = _terms(across)
    line = lax.broadcasted_iota(jnp.int32, (ROWS - SEQ, LOC), 0)
    terms = jnp.where(line == 0, hi, jnp.where(line == 1, mid, jnp.where(line == 2, low, 0.0)))
    out_ref[SEQ:] = terms.astype(BF)


def _own(h_ref):
    return h_ref[:, pl.ds(pl.multiple_of(_tp_index() * LOC, LOC), LOC)]


def _ff_in_first(tok_ref, w_ref, out_ref, w, sems):
    copies = [[], []]
    for part, cols in enumerate((slice(0, 2 * LOC), slice(2 * LOC, 3 * LOC))):
        for k in range(NZ):
            at = (slice(k * KB, (k + 1) * KB), cols)
            copies[part].append(pltpu.make_async_copy(w_ref.at[at], w.at[at], sems.at[part, k]))
            copies[part][k].start()
    both = _product_whole(tok_ref.at[:SEQ], w, 0, 2 * LOC, copies[0])
    out_ref[...] = (jax.nn.silu(both[:, :LOC]) * both[:, LOC:]).astype(BF)
    for copy in copies[1]:
        copy.wait()


def _ff_in_normed(pay_ref, gain_ref, w_ref, out_ref, own_ref, h_ref):
    _normed(pay_ref, gain_ref, 3, h_ref)
    own_ref[...] = _own(h_ref)
    both = _product_whole(h_ref, w_ref, 0, 2 * LOC)
    out_ref[...] = (jax.nn.silu(both[:, :LOC]) * both[:, LOC:]).astype(BF)


def _ff_down(hid_ref, own_ref, w_ref, out_ref):
    acc = _product_whole(hid_ref, w_ref, 2 * LOC, LOC)
    _payload(alpha_scale * own_ref[...].astype(F32) + 0.5 * acc, out_ref)


def _mix_down(hid_ref, own_ref, *rest):
    near, (far_ref, out_ref) = rest[:4], rest[4:]
    acc = _product_ring(hid_ref, near, far_ref, 2 * LOC, LOC)
    _payload(alpha_scale * own_ref[...].astype(F32) + acc, out_ref)


def _down_last(hid_ref, own_ref, w_ref, out_ref, stat_ref):
    acc = _product_whole(hid_ref, w_ref, 2 * LOC, LOC)
    total = alpha_scale * own_ref[...].astype(F32) + 0.5 * acc
    out_ref[...] = total
    cent = jnp.sum(total, axis=1, keepdims=True) / LOC
    dev = total - cent
    square = jnp.sum(dev * dev, axis=1, keepdims=True)
    lane = lax.broadcasted_iota(jnp.int32, (SEQ, 128), 1)
    stat_ref[...] = jnp.where(lane == 0, cent, jnp.where(lane == 1, square, 0.0))


def _mix_in(pay_ref, gain_ref, *rest):
    near, blocks, (out_ref, own_ref, far_ref, h_ref, sems) = rest[:4], rest[4:NZ], rest[NZ:]
    copies = [pltpu.make_async_copy(blocks[i], far_ref.at[i], sems.at[i]) for i in range(4)]
    for copy in copies:
        copy.start()
    _normed(pay_ref, gain_ref, 0, h_ref)
    own_ref[...] = _own(h_ref)
    both = _product_ring(h_ref, near, far_ref, 0, 2 * LOC, copies)
    stream = both[:, :LOC].astype(BF)
    gate = both[:, LOC:]
    window = lax.shift_left(jnp.int32(2), _tp_index())
    later = lax.broadcasted_iota(jnp.int32, (SEQ, SEQ), 0)
    earlier = lax.broadcasted_iota(jnp.int32, (SEQ, SEQ), 1)
    offset = later - earlier
    band = jnp.where((offset >= 0) & (offset < window), 1.0, 0.0).astype(BF)
    sums = _dot(band, stream)
    row = lax.broadcasted_iota(jnp.int32, (SEQ, 1), 0)
    counts = jnp.minimum(row + 1, window).astype(F32)
    pooled = sums / counts - stream.astype(F32)
    out_ref[...] = (pooled * jax.nn.silu(gate)).astype(BF)


def _call(kernel, outs, scratch, flops, args, in_hbm=(), limit_mib=6):
    full = pl.BlockSpec(memory_space=pltpu.VMEM)
    far = pl.BlockSpec(memory_space=pltpu.HBM)
    args_bytes = sum(a.size * a.dtype.itemsize for a in (*args, *in_hbm))
    return pl.pallas_call(
        kernel,
        out_shape=outs,
        in_specs=[full] * len(args) + [far] * len(in_hbm),
        out_specs=jax.tree.map(lambda _: full, outs),
        scratch_shapes=scratch,
        cost_estimate=pl.CostEstimate(
            flops=flops, bytes_accessed=args_bytes, transcendentals=0
        ),
        compiler_params=pltpu.CompilerParams(vmem_limit_bytes=limit_mib * 1024 * 1024),
    )(*args, *in_hbm)


def _terms(row):
    hi = row.astype(BF).astype(F32)
    mid = (row - hi).astype(BF).astype(F32)
    return hi, mid, row - hi - mid


def _pack(tok_ref, one_ref, two_ref, out_ref):
    out_ref[:SEQ] = tok_ref[...]
    line = lax.broadcasted_iota(jnp.int32, (ROWS - SEQ, LOC), 0)
    below = jnp.zeros((ROWS - SEQ, LOC), F32)
    for i, term in enumerate(_terms(one_ref[...]) + _terms(two_ref[...])):
        below = jnp.where(line == i, term, below)
    out_ref[SEQ:] = below.astype(BF)


def _sds(cols, dtype=BF, rows=SEQ):
    return jax.ShapeDtypeStruct((rows, cols), dtype)


ONE = 2 * SEQ * D * LOC


def _shift(value, axis, by):
    n = lax.axis_size(axis)
    return lax.ppermute(value, axis, [(i, (i + by) % n) for i in range(n)])


def _diagonal(value):
    pairs = [(y * NZ + (z + y) % NZ, y * NZ + z) for y in range(8) for z in range(NZ)]
    return lax.ppermute(value, ("rep", "z"), pairs)


def _cat(*values, axis=1):
    return jnp.concatenate(values, axis=axis)


def _over_xh(value):
    return lax.all_gather(value, "xh", axis=0, tiled=True)


def _y_ring(block):
    blocks = [None] * 8
    blocks[0] = block
    up = down = block
    for s in range(1, 5):
        down = _shift(down, "rep", -1)
        blocks[s] = down
        if s < 4:
            up = _shift(up, "rep", 1)
            blocks[8 - s] = up
    return blocks


def _whole(local_rows):
    return lax.all_gather(local_rows, ("xl", "co"), axis=1, tiled=True)


def shards(
    tokens, ff_first, ff_second, ff_down, mix_stream, mix_gate, mix_down, gain_one, gain_two, gain_three
):
    tok = tokens[0]
    diag = _diagonal(_cat(mix_stream, mix_gate, mix_down))
    x1 = _over_xh(_cat(ff_first, ff_second, ff_down))
    w_ff = lax.all_gather(x1, "z", axis=0, tiled=True)
    ring = _y_ring(_over_xh(diag))

    block = _call(_pack, _sds(LOC, rows=ROWS), [], 0, (tok, gain_one[None], gain_two[None]))
    whole = _whole(block)

    gains = whole[SEQ:]
    two = (_sds(LOC), _sds(LOC))
    h_scratch = [pltpu.VMEM((SEQ, D), BF)]

    outs = (_sds(LOC), _sds(3 * LOC, rows=D))
    sems = [pltpu.SemaphoreType.DMA((2, NZ))]
    hidden, w_ff = _call(_ff_in_first, outs, sems, 2 * ONE, (whole,), (w_ff,), 44)
    wide = _whole(hidden)
    pay = _call(_ff_down, _sds(LOC, rows=ROWS), [], ONE, (wide, tok, w_ff))

    wide = _whole(pay)
    near, far = [ring[k] for k in NEAR], [ring[k] for k in FAR]
    outs = (*two, jax.ShapeDtypeStruct((4, KB, 3 * LOC), BF))
    scratch = h_scratch + [pltpu.SemaphoreType.DMA((4,))]
    gated, first, far = _call(_mix_in, outs, scratch, 2 * ONE, (wide, gains, *near), far, 6)
    wide = _whole(gated)
    pay = _call(_mix_down, _sds(LOC, rows=ROWS), [], ONE, (wide, first, *near, far))

    wide = _whole(pay)
    hidden, second = _call(_ff_in_normed, two, h_scratch, 2 * ONE, (wide, gains, w_ff))
    wide = _whole(hidden)
    sums = (_sds(LOC, F32), _sds(128, F32))
    total, stats = _call(_down_last, sums, [], ONE, (wide, second, w_ff))

    every = lax.all_gather(stats[:, :2].T, ("xl", "co"), axis=0, tiled=False)
    cents, squares = every[:, 0], every[:, 1]
    mean = jnp.mean(cents, axis=0)
    var = (jnp.sum(squares, axis=0) + LOC * jnp.sum((cents - mean) ** 2, axis=0)) / D
    out = (total - mean[:, None]) * lax.rsqrt(var + norm_eps)[:, None] * gain_three[None, :]
    return out.astype(BF)[None]


def solution(mesh):
    fine = Mesh(mesh.devices.reshape(8, NZ, NX, 2, 2), ("rep", "z", "xh", "xl", "co"))
    rows, cols = ("z", "xh"), ("xl", "co")
    placed = (P(("rep", "z", "xh"), None, cols),) + (P(rows, cols),) * 6 + (P(cols),) * 3
    return jax.shard_map(
        shards, mesh=fine, in_specs=placed, out_specs=P(("rep", "z", "xh"), None, cols), check_vma=False
    )
```
